32 devices in a mesh: ep: 32 (over z, y, x, core).
Axes of the slice: x: 2, y: 2, z: 4, core: 2. Of those that a mesh axis runs over, the one named last changes fastest.
Arguments:
- tokens: bfloat16 [8192, 2048], P('ep'), may hold values from -6 to 6
- norm_gain: float32 [2048], replicated, may hold values from 0.5 to 1.5
- expert_ids: int32 [8192, 2], P('ep'), may hold values from 0 to 31, all different within a row; in each aligned block of 256 rows (0 to 255, 256 to 511, ...) at most 48 rows name the same one
- route_scores: float32 [8192, 2], P('ep'), may hold values from -6 to 6
- gate_weight: bfloat16 [32, 2048, 1536], P('ep'), may hold values from -0.125 to 0.125
- up_weight: bfloat16 [32, 2048, 1536], P('ep'), may hold values from -0.125 to 0.125
- down_weight: bfloat16 [32, 1536, 2048], P('ep'), may hold values from -0.15625 to 0.15625
Outputs:
- mixed: bfloat16 [8192, 2048], P('ep')
The draws below stay inside these ranges and needn't reach their ends.
Inputs may be any that keep to these rules, and one draw needn't show every extreme that they name: `expert_ids`: each row names 2 different experts. Among the 256 tokens of one device (each aligned block of 256 rows, in order) no expert is named by more than 48 tokens, a bound that some block reaches.
All inputs are finite; a program needn't handle non-finite values.
Results may differ from the reference program's by a relative error of at most 0.0025.
Values may be sent and summed in bfloat16 or wider, within the bound.
A program may use at most 128 MiB of HBM per device.

```python
import math
import jax
import jax.numpy as jnp
import numpy as np
from jax import lax

D = 2048
FF = 1536
TOP = 2
TOK_DEV = 256
EXPERTS = 32
CAP = 48
TOKENS = 8192


def level_of(rng, shape, split, least, top_value):
    level, own = 1.0, jax.random.fold_in(rng, 6)
    for axis_at, blocks in split:
        heights = jnp.exp(jax.random.uniform(jax.random.fold_in(own, axis_at), (blocks,), jnp.float32, least / len(split), top_value / len(split)))
        level = level * jnp.repeat(heights, shape[axis_at] // blocks).reshape([-1 if axis == axis_at else 1 for axis in range(len(shape))])
    return level


def routed_block(own_key, own, number, rows, amount, top, limit, skew):
    order = jax.random.permutation(own_key, amount)
    crowded, usual = load_shares(amount, rows * top, limit, skew, True), load_shares(amount, rows * top, limit, skew, False)
    places = jnp.arange(amount)

    def named(tallies, rotation):
        used = int((tallies > 0).sum())
        fixed = max(1, used // 4)
        moved = fixed + (places - fixed + rotation * (used - fixed)) % max(1, amount - fixed)
        return jnp.zeros((amount,), jnp.int32).at[order[jnp.where(places < fixed, places, moved)]].set(jnp.asarray(tallies, jnp.int32))

    tallies = jnp.where(number % 4 == 0, named(crowded, number // 4), named(usual, number - number // 4 - 1))
    mixed = jax.random.permutation(jax.random.fold_in(own, 3), amount)
    source_of, sink = mixed[0:amount // 2 * 2:2], mixed[1:amount // 2 * 2:2]
    slack = jnp.minimum(tallies[source_of] - 1, limit - tallies[sink]) // 2
    slack = jnp.where((source_of == order[0]) | (sink == order[0]) | (tallies[sink] == 0), 0, jnp.maximum(slack, 0))
    moved = jax.random.randint(jax.random.fold_in(own, 4), (amount // 2,), 0, 1 << 20) % (slack + 1)
    tallies = tallies.at[source_of].add(-moved).at[sink].add(moved)
    items = jnp.searchsorted(jnp.cumsum(tallies), jnp.arange(rows * top), side="right").astype(jnp.int32)
    listing = items.reshape(top, rows).T
    listing = listing[jax.random.permutation(jax.random.fold_in(own, 1), rows)]
    rotation = jax.random.randint(jax.random.fold_in(own, 2), (rows, 1), 0, top)
    return jnp.take_along_axis(listing, (jnp.arange(top)[None, :] + rotation) % top, axis=1)


def load_shares(count, total, bound, skew, full):
    weights = [(1 << 20) // math.isqrt(rank ** skew) + 1 for rank in range(1, count + 1)]
    largest = bound if full else min(bound, max(-(-total // count), total * weights[0] // sum(weights)))
    least = 1 if total - largest >= count - 1 else 0
    holding, surplus = [largest] + [least] * (count - 1), total - largest - least * (count - 1)
    while surplus > 0:
        candidates = [i for i in range(1, count) if holding[i] < largest] or [i for i in range(1, count) if holding[i] < bound]
        mass, left = sum([weights[i] for i in candidates]), surplus
        for i in candidates:
            addition = min(bound - holding[i], max(1, left * weights[i] // mass), surplus)
            holding[i] = holding[i] + addition
            surplus = surplus - addition
    return np.array(holding)


def noise(own_key, dims, deviation, limit, cuts=(), kind=jnp.bfloat16):
    values = deviation * jax.random.normal(own_key, dims, jnp.float32)
    if cuts:
        values = values * level_of(own_key, dims, cuts, -0.22, 0.18)
    return jnp.clip(values, -limit, limit).astype(kind)


def setup_inputs(seed: int = 0) -> dict:
    streams_of = jax.random.split(jax.random.key(seed), 8)
    tokens = noise(streams_of[0], (TOKENS, D), 1.0, 6.0, ((0, 32),))
    norm_gain = jnp.clip(1.0 + 0.1 * jax.random.normal(streams_of[1], (D,), jnp.float32), 0.5, 1.5)
    expert_ids_keys = jax.random.split(jax.random.fold_in(streams_of[2], 1), TOKENS // TOK_DEV)
    expert_ids_turns = jax.random.permutation(jax.random.fold_in(streams_of[2], 3), TOKENS // TOK_DEV)
    expert_ids = jax.vmap(lambda own, number: routed_block(jax.random.fold_in(streams_of[2], 2), own, number, TOK_DEV, EXPERTS, TOP, CAP, 2))(expert_ids_keys, expert_ids_turns).reshape((TOKENS, TOP))
    route_scores = noise(streams_of[3], (TOKENS, TOP), 1.0, 6.0, ((0, 32),), jnp.float32)
    gate_weight = noise(streams_of[4], (EXPERTS, D, FF), D ** -0.5, 0.125, ((0, 32),))
    up_weight = noise(streams_of[5], (EXPERTS, D, FF), D ** -0.5, 0.125, ((0, 32),))
    down_weight = noise(streams_of[6], (EXPERTS, FF, D), FF ** -0.5, 0.15625, ((0, 32),))
    return {"tokens": tokens, "norm_gain": norm_gain, "expert_ids": expert_ids, "route_scores": route_scores, "gate_weight": gate_weight, "up_weight": up_weight, "down_weight": down_weight}


eps_norm = 1e-05

def reference(tokens, norm_gain, expert_ids, route_scores, gate_weight, up_weight, down_weight):
    floats = tokens.astype(jnp.float32)
    scaled = floats * lax.rsqrt(lax.optimization_barrier(jnp.mean(floats * floats, axis=-1, keepdims=True)) + eps_norm)
    normed = (scaled * norm_gain).astype(jnp.bfloat16)
    flat_ids = expert_ids.reshape(-1).astype(jnp.int32)
    entries = TOKENS * TOP
    block_size = 128
    blocks = (entries + block_size - 1) // block_size + EXPERTS
    one_hot = (flat_ids[:, None] == jnp.arange(EXPERTS, dtype=jnp.int32)[None, :]).astype(jnp.int32)
    counts = lax.optimization_barrier(jnp.sum(one_hot, axis=0)).astype(jnp.int32)
    earlier = jnp.cumsum(one_hot, axis=0).astype(jnp.int32) - one_hot
    slot_rank = lax.optimization_barrier(jnp.sum(earlier * one_hot, axis=1)).astype(jnp.int32)
    padded_counts = ((counts + block_size - 1) // block_size * block_size).astype(jnp.int32)
    group_end = jnp.cumsum(padded_counts).astype(jnp.int32)
    group_start = (group_end - padded_counts).astype(jnp.int32)
    position = (group_start[flat_ids] + slot_rank).astype(jnp.int32)
    row_token = jnp.full((blocks * block_size,), TOKENS, jnp.int32)
    row_token = row_token.at[position].set(jnp.arange(entries, dtype=jnp.int32) // TOP)
    block_first = jnp.arange(blocks, dtype=jnp.int32) * block_size
    block_expert = lax.optimization_barrier(jnp.sum((group_end[None, :] <= block_first[:, None]).astype(jnp.int32), axis=1))
    block_expert = jnp.minimum(block_expert, EXPERTS - 1).astype(jnp.int32)
    padded = jnp.concatenate([normed, jnp.zeros((1, D), jnp.bfloat16)], axis=0)

    def run_block(block_pair):
        block_tokens, expert = block_pair
        inputs = padded[block_tokens]
        gate_pre = jnp.dot(inputs, gate_weight[expert], preferred_element_type=jnp.float32)
        up_pre = jnp.dot(inputs, up_weight[expert], preferred_element_type=jnp.float32)
        hidden = (jax.nn.silu(gate_pre) * up_pre).astype(jnp.bfloat16)
        return jnp.dot(hidden, down_weight[expert], preferred_element_type=jnp.float32).astype(jnp.bfloat16)
    outputs = lax.map(run_block, (row_token.reshape(blocks, block_size), block_expert))
    outputs = outputs.reshape(blocks * block_size, D)
    picked = outputs[position].reshape(TOKENS, TOP, D).astype(jnp.float32)
    mix_weights = jax.nn.softmax(route_scores, axis=-1)
    return lax.optimization_barrier(jnp.sum(mix_weights[:, :, None] * picked, axis=1)).astype(jnp.bfloat16)
```

```python
import jax
import jax.numpy as jnp
from jax import lax
from jax.sharding import PartitionSpec as P

eps_norm = 1e-05


def expert_hidden(gate_pre, up_pre):
    return (jax.nn.silu(gate_pre) * up_pre).astype(jnp.bfloat16)


def on_device(tokens, norm_gain, expert_ids, route_scores, gate_weight, up_weight, down_weight):
    devices = lax.axis_size("ep")
    half = devices // 2
    tok_count, top_count = expert_ids.shape
    capacity = max(1, 3 * tok_count * top_count // devices)
    slots = half * capacity
    me = lax.axis_index("ep")
    my_half = me // half
    across = [(i, (i + half) % devices) for i in range(devices)]
    groups = [list(range(half)), list(range(half, devices))]

    floats = tokens.astype(jnp.float32)
    scaled = floats * lax.rsqrt(jnp.mean(floats * floats, axis=-1, keepdims=True) + eps_norm)
    normed = (scaled * norm_gain).astype(jnp.bfloat16)
    far_normed = lax.ppermute(normed, "ep", across)

    flat_ids = expert_ids.reshape(-1)
    one_hot = (flat_ids[:, None] == jnp.arange(devices, dtype=jnp.int32)[None, :]).astype(jnp.int32)
    earlier = jnp.cumsum(one_hot, axis=0) - one_hot
    slot_rank = jnp.sum(earlier * one_hot, axis=1)
    position = (flat_ids * capacity + slot_rank).reshape(tok_count, top_count)
    mix_weights = jax.nn.softmax(route_scores, axis=-1)
    far_position = lax.ppermute(position, "ep", across)
    far_weights = lax.ppermute(mix_weights, "ep", across)

    gate_mat = gate_weight[0]
    up_mat = up_weight[0]
    down_mat = down_weight[0]

    near_at = position - my_half * slots
    far_at = far_position - my_half * slots

    def dispatch(rows, at):
        slot = jnp.arange(slots, dtype=jnp.int32)[:, None]
        chosen = slot == at[:, 0][None, :]
        for k in range(1, top_count):
            chosen = chosen | (slot == at[:, k][None, :])
        send = jnp.dot(
            chosen.astype(jnp.bfloat16), rows, preferred_element_type=jnp.float32
        ).astype(jnp.bfloat16)
        return lax.all_to_all(
            send, "ep", split_axis=0, concat_axis=0, tiled=True, axis_index_groups=groups
        )

    def experts(arrived):
        gate_pre = jnp.dot(arrived, gate_mat, preferred_element_type=jnp.float32)
        up_pre = jnp.dot(arrived, up_mat, preferred_element_type=jnp.float32)
        hidden = expert_hidden(gate_pre, up_pre)
        return jnp.dot(hidden, down_mat, preferred_element_type=jnp.float32).astype(jnp.bfloat16)

    def collect(results):
        return lax.all_to_all(
            results, "ep", split_axis=0, concat_axis=0, tiled=True, axis_index_groups=groups
        )

    def pick(back, at, k):
        slot = jnp.arange(slots, dtype=jnp.int32)[None, :]
        chosen = (slot == at[:, k][:, None]).astype(jnp.bfloat16)
        return jnp.dot(chosen, back, preferred_element_type=jnp.float32)

    near_arrived = dispatch(normed, near_at)
    far_arrived = dispatch(far_normed, far_at)
    far_back = collect(experts(far_arrived))
    near_back = collect(experts(near_arrived))

    far_in = (far_at >= 0) & (far_at < slots)
    far_all = jnp.all(far_in, axis=1, keepdims=True)
    far_coef = jnp.where(far_all, far_weights, far_in.astype(jnp.float32))
    reply = sum(far_coef[:, k][:, None] * pick(far_back, far_at, k) for k in range(top_count))
    reply = lax.ppermute(reply.astype(jnp.bfloat16), "ep", across)

    near_in = (near_at >= 0) & (near_at < slots)
    none_near = ~jnp.any(near_in, axis=1)
    reply_coef = jnp.sum(jnp.where(near_in, 0.0, mix_weights), axis=1)
    reply_coef = jnp.where(none_near, 1.0, reply_coef)
    total = sum(mix_weights[:, k][:, None] * pick(near_back, near_at, k) for k in range(top_count))
    return (total + reply_coef[:, None] * reply.astype(jnp.float32)).astype(jnp.bfloat16)


def solution(mesh):
    placed = (
        P("ep", None),
        P(),
        P("ep", None),
        P("ep", None),
        P("ep", None, None),
        P("ep", None, None),
        P("ep", None, None),
    )
    return jax.shard_map(
        on_device, mesh=mesh, in_specs=placed, out_specs=P("ep", None), check_vma=False
    )
```

```python
import jax
import jax.numpy as jnp
from jax import lax
from jax.sharding import PartitionSpec as P

eps_norm = 1e-05


def expert_hidden(gate_pre, up_pre):
    return (jax.nn.silu(gate_pre) * up_pre).astype(jnp.bfloat16)


def on_device(tokens, norm_gain, expert_ids, route_scores, gate_weight, up_weight, down_weight):
    devices = lax.axis_size("ep")
    half = devices // 2
    tok_count, top_count = expert_ids.shape
    capacity = max(1, 3 * tok_count * top_count // devices)
    slots = half * capacity
    me = lax.axis_index("ep")
    my_half = me // half
    across = [(i, (i + half) % devices) for i in range(devices)]
    groups = [list(range(half)), list(range(half, devices))]

    floats = tokens.astype(jnp.float32)
    scaled = floats * lax.rsqrt(jnp.mean(floats * floats, axis=-1, keepdims=True) + eps_norm)
    normed = (scaled * norm_gain).astype(jnp.bfloat16)
    far_normed = lax.ppermute(normed, "ep", across)

    flat_ids = expert_ids.reshape(-1)
    one_hot = (flat_ids[:, None] == jnp.arange(devices, dtype=jnp.int32)[None, :]).astype(jnp.int32)
    earlier = jnp.cumsum(one_hot, axis=0) - one_hot
    slot_rank = jnp.sum(earlier * one_hot, axis=1)
    position = (flat_ids * capacity + slot_rank).reshape(tok_count, top_count)
    mix_weights = jax.nn.softmax(route_scores, axis=-1)
    plan = jnp.concatenate([position.astype(jnp.float32), mix_weights], axis=1)
    far_plan = lax.ppermute(plan, "ep", across)

    gate_mat = gate_weight[0]
    up_mat = up_weight[0]
    down_mat = down_weight[0]

    near_at = position - my_half * slots

    def dispatch(rows, at):
        slot = jnp.arange(slots, dtype=jnp.int32)[:, None]
        chosen = slot == at[:, 0][None, :]
        for k in range(1, top_count):
            chosen = chosen | (slot == at[:, k][None, :])
        send = jnp.dot(
            chosen.astype(jnp.bfloat16), rows, preferred_element_type=jnp.float32
        ).astype(jnp.bfloat16)
        return lax.all_to_all(
            send, "ep", split_axis=0, concat_axis=0, tiled=True, axis_index_groups=groups
        )

    def experts(arrived):
        gate_pre = jnp.dot(arrived, gate_mat, preferred_element_type=jnp.float32)
        up_pre = jnp.dot(arrived, up_mat, preferred_element_type=jnp.float32)
        hidden = expert_hidden(gate_pre, up_pre)
        return jnp.dot(hidden, down_mat, preferred_element_type=jnp.float32).astype(jnp.bfloat16)

    def collect(results):
        return lax.all_to_all(
            results, "ep", split_axis=0, concat_axis=0, tiled=True, axis_index_groups=groups
        )

    def pick(back, at, k):
        slot = jnp.arange(slots, dtype=jnp.int32)[None, :]
        chosen = (slot == at[:, k][:, None]).astype(jnp.bfloat16)
        return jnp.dot(chosen, back, preferred_element_type=jnp.float32)

    near_arrived = dispatch(normed, near_at)
    near_arrived, far_normed, far_plan = lax.optimization_barrier((near_arrived, far_normed, far_plan))
    far_position = far_plan[:, :top_count].astype(jnp.int32)
    far_weights = far_plan[:, top_count:]
    far_at = far_position - my_half * slots
    far_arrived = dispatch(far_normed, far_at)
    near_results = experts(near_arrived)
    far_arrived, near_results = lax.optimization_barrier((far_arrived, near_results))
    far_back = collect(experts(far_arrived))
    far_back, near_results = lax.optimization_barrier((far_back, near_results))
    near_back = collect(near_results)

    far_in = (far_at >= 0) & (far_at < slots)
    far_all = jnp.all(far_in, axis=1, keepdims=True)
    far_coef = jnp.where(far_all, far_weights, far_in.astype(jnp.float32))
    reply = sum(far_coef[:, k][:, None] * pick(far_back, far_at, k) for k in range(top_count))
    reply = lax.ppermute(reply.astype(jnp.bfloat16), "ep", across)

    near_in = (near_at >= 0) & (near_at < slots)
    none_near = ~jnp.any(near_in, axis=1)
    reply_coef = jnp.sum(jnp.where(near_in, 0.0, mix_weights), axis=1)
    reply_coef = jnp.where(none_near, 1.0, reply_coef)
    total = sum(mix_weights[:, k][:, None] * pick(near_back, near_at, k) for k in range(top_count))
    return (total + reply_coef[:, None] * reply.astype(jnp.float32)).astype(jnp.bfloat16)


def solution(mesh):
    placed = (
        P("ep", None),
        P(),
        P("ep", None),
        P("ep", None),
        P("ep", None, None),
        P("ep", None, None),
        P("ep", None, None),
    )
    return jax.shard_map(
        on_device, mesh=mesh, in_specs=placed, out_specs=P("ep", None), check_vma=False
    )
```

```python
import jax
import jax.numpy as jnp
from jax import lax
from jax.sharding import PartitionSpec as P

eps_norm = 1e-05


def expert_hidden(gate_pre, up_pre):
    return (jax.nn.silu(gate_pre) * up_pre).astype(jnp.bfloat16)


def on_device(tokens, norm_gain, expert_ids, route_scores, gate_weight, up_weight, down_weight):
    devices = lax.axis_size("ep")
    half = devices // 2
    tok_count, top_count = expert_ids.shape
    capacity = max(1, 3 * tok_count * top_count // devices)
    slots = half * capacity
    me = lax.axis_index("ep")
    my_half = me // half
    across = [(i, (i + half) % devices) for i in range(devices)]
    groups = [list(range(half)), list(range(half, devices))]

    floats = tokens.astype(jnp.float32)
    scaled = floats * lax.rsqrt(jnp.mean(floats * floats, axis=-1, keepdims=True) + eps_norm)
    normed = (scaled * norm_gain).astype(jnp.bfloat16)
    far_normed = lax.ppermute(normed, "ep", across)

    flat_ids = expert_ids.reshape(-1)
    one_hot = (flat_ids[:, None] == jnp.arange(devices, dtype=jnp.int32)[None, :]).astype(jnp.int32)
    earlier = jnp.cumsum(one_hot, axis=0) - one_hot
    slot_rank = jnp.sum(earlier * one_hot, axis=1)
    position = (flat_ids * capacity + slot_rank).reshape(tok_count, top_count)
    mix_weights = jax.nn.softmax(route_scores, axis=-1)
    plan = jnp.concatenate([position.astype(jnp.float32), mix_weights], axis=1)
    far_plan = lax.ppermute(plan, "ep", across)

    gate_mat = gate_weight[0]
    up_mat = up_weight[0]
    down_mat = down_weight[0]

    near_at = position - my_half * slots

    def dispatch(rows, at, first, last):
        own = jnp.arange(half, dtype=jnp.int32)[:, None] * capacity
        slot = (own + jnp.arange(first, last, dtype=jnp.int32)[None, :]).reshape(-1, 1)
        chosen = slot == at[:, 0][None, :]
        for k in range(1, top_count):
            chosen = chosen | (slot == at[:, k][None, :])
        send = jnp.dot(
            chosen.astype(jnp.bfloat16), rows, preferred_element_type=jnp.float32
        ).astype(jnp.bfloat16)
        return lax.all_to_all(
            send, "ep", split_axis=0, concat_axis=0, tiled=True, axis_index_groups=groups
        )

    def experts(arrived):
        gate_pre = jnp.dot(arrived, gate_mat, preferred_element_type=jnp.float32)
        up_pre = jnp.dot(arrived, up_mat, preferred_element_type=jnp.float32)
        hidden = expert_hidden(gate_pre, up_pre)
        return jnp.dot(hidden, down_mat, preferred_element_type=jnp.float32).astype(jnp.bfloat16)

    def collect(results):
        return lax.all_to_all(
            results, "ep", split_axis=0, concat_axis=0, tiled=True, axis_index_groups=groups
        )

    def pick(back, at, k):
        slot = jnp.arange(slots, dtype=jnp.int32)[None, :]
        chosen = (slot == at[:, k][:, None]).astype(jnp.bfloat16)
        return jnp.dot(chosen, back, preferred_element_type=jnp.float32)

    cut = capacity // 2
    early_arrived = dispatch(normed, near_at, 0, cut)
    early_arrived, far_normed, far_plan = lax.optimization_barrier((early_arrived, far_normed, far_plan))
    far_position = far_plan[:, :top_count].astype(jnp.int32)
    far_weights = far_plan[:, top_count:]
    far_at = far_position - my_half * slots
    far_arrived = dispatch(far_normed, far_at, 0, capacity)
    early_results = experts(early_arrived)
    far_arrived, early_results, near_rows = lax.optimization_barrier((far_arrived, early_results, normed))
    late_arrived = dispatch(near_rows, near_at, cut, capacity)
    far_results = experts(far_arrived)
    far_results, late_arrived = lax.optimization_barrier((far_results, late_arrived))
    far_back = collect(far_results)
    late_results = experts(late_arrived)
    near_results = jnp.concatenate(
        [early_results.reshape(half, cut, -1), late_results.reshape(half, capacity - cut, -1)], axis=1
    ).reshape(slots, -1)
    far_back, near_results = lax.optimization_barrier((far_back, near_results))
    near_back = collect(near_results)

    far_in = (far_at >= 0) & (far_at < slots)
    far_all = jnp.all(far_in, axis=1, keepdims=True)
    far_coef = jnp.where(far_all, far_weights, far_in.astype(jnp.float32))
    reply = sum(far_coef[:, k][:, None] * pick(far_back, far_at, k) for k in range(top_count))
    reply = lax.ppermute(reply.astype(jnp.bfloat16), "ep", across)

    near_in = (near_at >= 0) & (near_at < slots)
    none_near = ~jnp.any(near_in, axis=1)
    reply_coef = jnp.sum(jnp.where(near_in, 0.0, mix_weights), axis=1)
    reply_coef = jnp.where(none_near, 1.0, reply_coef)
    total = sum(mix_weights[:, k][:, None] * pick(near_back, near_at, k) for k in range(top_count))
    return (total + reply_coef[:, None] * reply.astype(jnp.float32)).astype(jnp.bfloat16)


def solution(mesh):
    placed = (
        P("ep", None),
        P(),
        P("ep", None),
        P("ep", None),
        P("ep", None, None),
        P("ep", None, None),
        P("ep", None, None),
    )
    return jax.shard_map(
        on_device, mesh=mesh, in_specs=placed, out_specs=P("ep", None), check_vma=False
    )
```
